32 devices in a mesh: sp: 8 (over z, y), fs: 2 (over x), tp: 2 (over core).
Axes of the slice: x: 2, y: 2, z: 4, core: 2. Of those that a mesh axis runs over, the one named last changes fastest.
Arguments:
- ret_query: bfloat16 [1024, 2, 512], P('sp', 'fs', 'tp'), may hold values from -6 to 6
- ret_key: bfloat16 [1024, 2, 512], P('sp', 'fs', 'tp'), may hold values from -6 to 6
- ret_value: bfloat16 [1024, 2, 1024], P('sp', 'fs', 'tp'), may hold values from -6 to 6
- log_decay: float32 [2, 4, 1024], P('fs', 'tp', 'sp'), may hold values from -1.2 to 0
- ret_gain: float32 [1024], P('tp'), may hold values from 0.1 to 1.9
- mla_query: bfloat16 [1024, 2, 1536], P('sp', 'fs', 'tp'), may hold values from -64 to 64
- kv_latent: bfloat16 [1024, 2, 256], P('sp', 'fs'), may hold values from -6 to 6
- rope_key: bfloat16 [1024, 2, 64], P('sp', 'fs'), may hold values from -8 to 8
- key_up: bfloat16 [256, 1024], replicated, may hold values from -0.375 to 0.375
- value_up: bfloat16 [256, 1024], replicated, may hold values from -3 to 3
- ret_out: bfloat16 [1024, 2048], P('tp', 'fs'), may hold values from -0.1875 to 0.1875
- mla_out: bfloat16 [1024, 2048], P('tp', 'fs'), may hold values from -0.1875 to 0.1875
Outputs:
- mixed_rows: bfloat16 [1024, 2, 2048], P(('sp', 'tp'), 'fs')
- log_weight: float32 [2, 8, 1024], P('fs', 'tp', 'sp')
The draws below stay inside these ranges and needn't reach their ends.
All inputs are finite; a program needn't handle non-finite values.
Results may differ from the reference program's by a relative error of at most 0.014.
Values may be sent and summed in bfloat16 or wider, within the bound.
No kernel may reach another device: no remote copies, remote signals or barrier semaphores. Data moves between devices by JAX's collectives and lax.ppermute only.
A program may use at most 128 MiB of HBM per device.

```python
import math
import jax
import jax.numpy as jnp
from jax import lax

D = 2048
RH = 4
QK = 128
VD = 256
MH = 8
NOPE = 128
ROPE = 64
VDM = 128
KVR = 256
BLOCK = 128
SEQUENCE_LENGTH = 1024
SEQUENCE_COUNT = 2
N_TP = 2


def draw_log_decay(key, part):
    quick_rate_key, factor_key, spike_key, dropout_key = jax.random.split(jax.random.fold_in(key, 3), 4)
    fast_share = 0.5
    fast_heads = jax.random.uniform(quick_rate_key, (SEQUENCE_COUNT, RH, 1)) < fast_share
    blocks = SEQUENCE_LENGTH // BLOCK
    factor = jax.random.uniform(factor_key, (SEQUENCE_COUNT, RH, blocks), jnp.float32, 0.4, 1.0)
    factor = jnp.repeat(factor, BLOCK, axis=2)
    slow_rate = 0.5 * math.log(10.0) / SEQUENCE_LENGTH
    fast_rate = math.log(10.0) / 40.0
    decay_rates = jnp.where(fast_heads, fast_rate, slow_rate) * factor
    spike_rows = jax.random.randint(spike_key, (SEQUENCE_COUNT, 1, 2), 0, SEQUENCE_LENGTH)
    dropped_entries = jax.random.uniform(dropout_key, (SEQUENCE_COUNT, RH, 2), jnp.float32, 0.2, 0.4)
    total_step_rows = jnp.arange(SEQUENCE_LENGTH)
    removed_mask = total_step_rows[None, None, :, None] == spike_rows[:, :, None, :]
    spike_draws = jnp.sum(jnp.where(removed_mask, jnp.log(1.0 - dropped_entries)[:, :, None, :], 0.0), axis=-1)
    return (spike_draws - decay_rates).astype(jnp.float32)


def draw_rope_key(key, part):
    noise_draw = jax.random.normal(jax.random.fold_in(key, 11), (SEQUENCE_LENGTH, SEQUENCE_COUNT, ROPE), jnp.float32)
    base_draw = jnp.clip(noise_draw, -4.0, 4.0)
    return base_draw.astype(jnp.bfloat16)


def draw_mla_query(key, part):
    noise_draw = jax.random.normal(jax.random.fold_in(key, 13), (SEQUENCE_LENGTH, SEQUENCE_COUNT, MH, NOPE + ROPE), jnp.float32)
    base_draw = jnp.clip(noise_draw, -6.0, 6.0)
    return base_draw.reshape(SEQUENCE_LENGTH, SEQUENCE_COUNT, MH * (NOPE + ROPE)).astype(jnp.bfloat16)


def levels(stream_key, shape, cuts, least, largest):
    loudness, own = 1.0, jax.random.fold_in(stream_key, 6)
    for position, shards_of in cuts:
        steps = jnp.exp(jax.random.uniform(jax.random.fold_in(own, position), (shards_of,), jnp.float32, least / len(cuts), largest / len(cuts)))
        loudness = loudness * jnp.repeat(steps, shape[position] // shards_of).reshape([-1 if axis == position else 1 for axis in range(len(shape))])
    return loudness


def bell_draw(stream_key, shape, deviation, limit, pieces=(), kind=jnp.bfloat16):
    drawn = deviation * jax.random.normal(stream_key, shape, jnp.float32)
    if pieces:
        drawn = drawn * levels(stream_key, shape, pieces, -0.22, 0.18)
    return jnp.clip(drawn, -limit, limit).astype(kind)


def setup_inputs(seed: int = 0) -> dict:
    seeds = jax.random.split(jax.random.key(seed), 13)
    ret_query = bell_draw(seeds[0], (SEQUENCE_LENGTH, SEQUENCE_COUNT, RH * QK), 1.0, 6.0, ((0, 8), (1, 2), (2, 2)))
    ret_key = bell_draw(seeds[1], (SEQUENCE_LENGTH, SEQUENCE_COUNT, RH * QK), 1.0, 6.0, ((0, 8), (1, 2), (2, 2)))
    ret_value = bell_draw(seeds[2], (SEQUENCE_LENGTH, SEQUENCE_COUNT, RH * VD), 1.0, 6.0, ((0, 8), (1, 2), (2, 2)))
    log_decay = draw_log_decay(jax.random.fold_in(seeds[12], 71), 0)
    ret_gain = jnp.clip(1.0 + 0.18 * jax.random.normal(seeds[4], (RH * VD,), jnp.float32), 0.1, 1.9)
    mla_query = draw_mla_query(jax.random.fold_in(seeds[12], 71), 0)
    kv_latent = bell_draw(seeds[6], (SEQUENCE_LENGTH, SEQUENCE_COUNT, KVR), 1.0, 6.0, ((0, 8), (1, 2)))
    rope_key = draw_rope_key(jax.random.fold_in(seeds[12], 71), 0)
    key_up = bell_draw(seeds[8], (KVR, MH * NOPE), KVR ** -0.5, 0.375)
    value_up = bell_draw(seeds[9], (KVR, MH * VDM), 4 ** -0.5, 3.0)
    ret_out = bell_draw(seeds[10], (RH * VD, D), (RH * VD) ** -0.5, 0.1875, ((0, 2), (1, 2)))
    mla_out = bell_draw(seeds[11], (MH * VDM, D), (MH * VDM) ** -0.5, 0.1875, ((0, 2), (1, 2)))
    return dict(ret_query=ret_query, ret_key=ret_key, ret_value=ret_value, log_decay=log_decay, ret_gain=ret_gain, mla_query=mla_query, kv_latent=kv_latent, rope_key=rope_key, key_up=key_up, value_up=value_up, ret_out=ret_out, mla_out=mla_out)


def rotate(vectors, positions):
    half_width = vectors.shape[-1] // 2
    inverse = 1.0 / 10000.0 ** (jnp.arange(half_width, dtype=jnp.float32) / half_width)
    angles = positions.astype(jnp.float32)[:, None] * inverse[None, :]
    cosine = jnp.cos(angles)[:, None, None, :]
    sine_part = jnp.sin(angles)[:, None, None, :]
    widened = vectors.astype(jnp.float32)
    front_part = widened[..., :half_width]
    back_part = widened[..., half_width:]
    turned = jnp.concatenate([front_part * cosine - back_part * sine_part, front_part * sine_part + back_part * cosine], axis=-1)
    return turned.astype(jnp.bfloat16)

def retention_block(state, inputs):
    queries, key_rows, value_rows, decay_rows = inputs
    span_rows = queries.shape[0]
    logit_scale = QK ** (-0.5)
    cumulative = jnp.cumsum(decay_rows, axis=-1)
    log_gap = cumulative[..., :, None] - cumulative[..., None, :]
    causal = jnp.tril(jnp.ones((span_rows, span_rows), dtype=bool))
    score_matrix = jnp.einsum('ishd,jshd->shij', queries.astype(jnp.float32), key_rows.astype(jnp.float32)) * logit_scale
    weights = jnp.where(causal, score_matrix * jnp.exp(jnp.where(causal, log_gap, 0.0)), 0.0).astype(jnp.bfloat16)
    intra_block = jnp.einsum('shij,jshe->ishe', weights.astype(jnp.float32), value_rows.astype(jnp.float32))
    growth = jnp.transpose(jnp.exp(cumulative), (2, 0, 1))[..., None]
    cross_term = jnp.einsum('ishd,shde->ishe', queries.astype(jnp.float32), state, precision=lax.Precision.HIGHEST) * logit_scale * growth
    tail_decay = jnp.transpose(jnp.exp(cumulative[..., -1:] - cumulative), (2, 0, 1))[..., None]
    block_state = jnp.einsum('jshd,jshe->shde', key_rows.astype(jnp.float32) * tail_decay, value_rows.astype(jnp.float32), precision=lax.Precision.HIGHEST)
    next_state = state * jnp.exp(cumulative[..., -1])[..., None, None] + block_state
    return (next_state, intra_block + cross_term)

def reference(ret_query, ret_key, ret_value, log_decay, ret_gain, mla_query, kv_latent, rope_key, key_up, value_up, ret_out, mla_out):
    length = ret_query.shape[0]
    groups = ret_query.shape[1]
    positions = jnp.arange(length, dtype=jnp.int32)
    queries = rotate(ret_query.reshape(length, groups, RH, QK), positions)
    key_rows = rotate(ret_key.reshape(length, groups, RH, QK), positions)
    value_rows = ret_value.reshape(length, groups, RH, VD)
    blocks = length // BLOCK
    decay_blocks = jnp.transpose(log_decay.reshape(groups, RH, blocks, BLOCK), (2, 0, 1, 3))
    initial = jnp.zeros((groups, RH, QK, VD), jnp.float32)
    _, retained = lax.scan(retention_block, initial, (queries.reshape(blocks, BLOCK, groups, RH, QK), key_rows.reshape(blocks, BLOCK, groups, RH, QK), value_rows.reshape(blocks, BLOCK, groups, RH, VD), decay_blocks))
    retained = retained.reshape(length, groups, RH, VD)
    normed = retained * lax.rsqrt(lax.optimization_barrier(jnp.mean(retained * retained, axis=-1, keepdims=True)) + 1e-06) * ret_gain.reshape(RH, VD)
    ret_heads = normed.astype(jnp.bfloat16).reshape(length, groups, RH * VD)
    head_rows = mla_query.reshape(length, groups, MH, NOPE + ROPE)
    query_rope = rotate(head_rows[..., NOPE:], positions)
    key_rope = rotate(rope_key[:, :, None, :], positions)[:, :, 0, :]
    absorbed = jnp.einsum('lshn,chn->lshc', head_rows[..., :NOPE].astype(jnp.float32), key_up.reshape(KVR, MH, NOPE).astype(jnp.float32)).astype(jnp.bfloat16)
    latent_width = kv_latent.astype(jnp.float32)
    rotary_width = key_rope.astype(jnp.float32)
    logit_scale = (NOPE + ROPE) ** (-0.5)
    rows_block = math.gcd(length, 128)

    def query_block(block_index):
        begin_row = block_index * rows_block
        absorbed_block_scores = lax.dynamic_slice_in_dim(absorbed, begin_row, rows_block, 0).astype(jnp.float32)
        rotary_block_scores = lax.dynamic_slice_in_dim(query_rope, begin_row, rows_block, 0).astype(jnp.float32)
        score_matrix = (jnp.einsum('uoda,voa->oduv', absorbed_block_scores, latent_width) + jnp.einsum('covw,zow->ovcz', rotary_block_scores, rotary_width)) * logit_scale
        query_positions = begin_row + jnp.arange(rows_block, dtype=jnp.int32)
        visible = positions[None, :] <= query_positions[:, None]
        score_matrix = jnp.where(visible, score_matrix, -jnp.inf)
        row_max = lax.optimization_barrier(jnp.max(score_matrix, axis=-1))
        exponent = jnp.exp(score_matrix - row_max[..., None])
        total = lax.optimization_barrier(jnp.sum(exponent, axis=-1))
        rounded = lax.optimization_barrier(exponent.astype(jnp.bfloat16))
        weighted = jnp.einsum('shbl,lsc->shbc', rounded.astype(jnp.float32), latent_width)
        latent_mean = (weighted / total[..., None]).astype(jnp.bfloat16)
        return (latent_mean, row_max + jnp.log(total))
    means, log_rows = lax.map(query_block, jnp.arange(length // rows_block, dtype=jnp.int32))
    means = jnp.transpose(means, (1, 2, 0, 3, 4)).reshape(groups, MH, length, KVR)
    log_weight = jnp.transpose(log_rows, (1, 2, 0, 3)).reshape(groups, MH, length)
    mla_heads = jnp.einsum('shlc,chv->lshv', means.astype(jnp.float32), value_up.reshape(KVR, MH, VDM).astype(jnp.float32)).astype(jnp.bfloat16).reshape(length, groups, MH * VDM)
    ret_width = RH * VD // N_TP
    mla_width = MH * VDM // N_TP
    flat_ret = ret_heads.reshape(length * groups, RH * VD)
    flat_mla = mla_heads.reshape(length * groups, MH * VDM)
    summed = jnp.zeros((length * groups, ret_out.shape[1]), jnp.float32)
    for group_index in range(N_TP):
        partial_value = jnp.dot(flat_ret[:, group_index * ret_width:(group_index + 1) * ret_width], ret_out[group_index * ret_width:(group_index + 1) * ret_width], preferred_element_type=jnp.float32)
        partial_value = partial_value + jnp.dot(flat_mla[:, group_index * mla_width:(group_index + 1) * mla_width], mla_out[group_index * mla_width:(group_index + 1) * mla_width], preferred_element_type=jnp.float32)
        rounded_part = lax.optimization_barrier(partial_value.astype(jnp.bfloat16))
        summed = summed + rounded_part.astype(jnp.float32)
    mixed_rows = summed.astype(jnp.bfloat16).reshape(length, groups, ret_out.shape[1])
    return (mixed_rows, log_weight)
```

```python
import jax
import jax.numpy as jnp
from jax import lax
from jax.sharding import PartitionSpec as P

QK = 128
VD = 256
NOPE = 128
ROPE = 64
VDM = 128
KVR = 256
F32 = jnp.float32
BF16 = jnp.bfloat16


def swap(x, axis, distance):
    size = lax.axis_size(axis)
    return lax.ppermute(x, axis, [(i, i ^ distance) for i in range(size)])


def angles_of(positions, half_width):
    inverse = 1.0 / 10000.0 ** (jnp.arange(half_width, dtype=F32) / half_width)
    angles = positions.astype(F32)[:, None] * inverse[None, :]
    return jnp.cos(angles), jnp.sin(angles)


def rotate(vectors, cosine, sine):
    half_width = vectors.shape[-1] // 2
    wide = vectors.astype(F32)
    front, back = wide[..., :half_width], wide[..., half_width:]
    return jnp.concatenate([front * cosine - back * sine, front * sine + back * cosine], axis=-1).astype(BF16)


def dot(a, b, dims=((1,), (0,))):
    return lax.dot_general(a, b, (dims, ((), ())), preferred_element_type=F32)


def gather_keys(own):
    n = lax.axis_size("sp")
    place = lax.axis_index("sp")
    if n != 8 or lax.axis_size("tp") != 2:
        every = lax.all_gather(own, "sp", axis=0, tiled=False)
        return list(every), [jnp.int32(j) for j in range(n)]
    core = lax.axis_index("tp")
    got = []
    for step in (1, 3, 5):
        perm = [(2 * i + t, 2 * (i ^ (step + t)) + t) for i in range(n) for t in range(2)]
        got.append(lax.ppermute(own, ("sp", "tp"), perm))
    last = swap(own, "sp", 7)
    other = swap(jnp.concatenate(got, axis=0), "tp", 1)
    rows = own.shape[0]
    pieces = [own, last] + got + [other[rows * k : rows * (k + 1)] for k in range(3)]
    steps = [jnp.int32(0), jnp.int32(7)] + [s + core for s in (1, 3, 5)] + [s + 1 - core for s in (1, 3, 5)]
    return pieces, [place ^ s for s in steps]


def entering_state(state, log_total):
    n = lax.axis_size("sp")
    place = lax.axis_index("sp")
    heads = state.shape[0]
    total, total_log = state, log_total
    before = jnp.zeros_like(state)
    before_log = jnp.zeros_like(log_total)
    distance = 1
    while distance < n:
        high = lax.reduce_precision(total_log, 8, 7)
        pair = jnp.stack([high, total_log - high], axis=0)
        tail = jnp.broadcast_to(jnp.pad(pair, ((0, 6), (0, 0)))[:, :, None], (8, heads, VD // heads)).reshape(8, VD)
        message = jnp.concatenate([total.astype(BF16).reshape(heads * QK, VD), tail.astype(BF16)], axis=0)
        seen = swap(message, "sp", distance)
        seen_total = seen[: heads * QK].astype(F32).reshape(heads, QK, VD)
        logs = seen[heads * QK : heads * QK + 2].astype(F32)
        seen_log = jnp.sum(logs, axis=0)[:: VD // heads]
        upper = (place & distance) != 0
        before = jnp.where(upper, before + jnp.exp(before_log)[:, None, None] * seen_total, before)
        before_log = jnp.where(upper, before_log + seen_log, before_log)
        if 2 * distance < n:
            early = jnp.where(upper, seen_total, total)
            late = jnp.where(upper, total, seen_total)
            late_log = jnp.where(upper, total_log, seen_log)
            total = jnp.exp(late_log)[:, None, None] * early + late
            total_log = total_log + seen_log
        distance *= 2
    return before


def on_device(
    ret_query, ret_key, ret_value, log_decay, ret_gain, mla_query,
    kv_latent, rope_key, key_up, value_up, ret_out, mla_out,
):
    rows = ret_query.shape[0]
    ret_local = ret_value.shape[2] // VD
    mla_local = mla_query.shape[2] // (NOPE + ROPE)
    core = lax.axis_index("tp")
    place = lax.axis_index("sp")
    fs_size = lax.axis_size("fs")
    positions = place * rows + jnp.arange(rows, dtype=jnp.int32)
    if fs_size == 2:
        far_ret, far_mla = swap(ret_out, "fs", 1), swap(mla_out, "fs", 1)
    else:
        far_ret = lax.all_gather(ret_out, "fs", axis=1, tiled=True)
        far_mla = lax.all_gather(mla_out, "fs", axis=1, tiled=True)

    cos_a, sin_a = angles_of(positions, ROPE // 2)
    own_rope = rotate(rope_key[:, 0], cos_a, sin_a)
    own = jnp.concatenate([kv_latent[:, 0], own_rope, jnp.zeros((rows, 128 - ROPE), BF16)], axis=-1)
    pieces, blocks = gather_keys(own)

    cos_r, sin_r = angles_of(positions, QK // 2)
    cumulative = jnp.cumsum(log_decay[0], axis=-1)
    rq = [rotate(ret_query[:, 0, h * QK : (h + 1) * QK], cos_r, sin_r) for h in range(ret_local)]
    rk = [rotate(ret_key[:, 0, h * QK : (h + 1) * QK], cos_r, sin_r) for h in range(ret_local)]
    rv = [ret_value[:, 0, h * VD : (h + 1) * VD] for h in range(ret_local)]
    tail = jnp.exp(cumulative[:, -1:] - cumulative)
    state = jnp.stack(
        [dot((rk[h].astype(F32) * tail[h][:, None]).astype(BF16), rv[h], ((0,), (0,))) for h in range(ret_local)]
    )
    carried = entering_state(state, cumulative[:, -1])

    scale = QK ** (-0.5)
    causal = jnp.tril(jnp.ones((rows, rows), dtype=bool))
    ret_heads = []
    intra = []
    for h in range(ret_local):
        gap = cumulative[h][:, None] - cumulative[h][None, :]
        score = dot(rq[h], rk[h], ((1,), (1,))) * scale
        weight = jnp.where(causal, score * jnp.exp(jnp.where(causal, gap, 0.0)), 0.0).astype(BF16)
        intra.append(dot(weight, rv[h]))

    head_rows = mla_query[:, 0].reshape(rows, mla_local, NOPE + ROPE)
    up_keys = lax.dynamic_slice_in_dim(key_up, core * (mla_local * NOPE), mla_local * NOPE, 1)
    up_values = lax.dynamic_slice_in_dim(value_up, core * (mla_local * VDM), mla_local * VDM, 1)
    q_parts = []
    for h in range(mla_local):
        absorbed = dot(head_rows[:, h, :NOPE], up_keys[:, h * NOPE : (h + 1) * NOPE], ((1,), (1,))).astype(BF16)
        aq = rotate(head_rows[:, h, NOPE:], cos_a, sin_a)
        q_parts.append(jnp.concatenate([absorbed, aq, jnp.zeros((rows, 128 - ROPE), BF16)], axis=-1))
    q_all = jnp.concatenate(q_parts, axis=0)
    keys = jnp.concatenate(pieces, axis=0)
    key_positions = jnp.concatenate([b * rows + jnp.arange(rows, dtype=jnp.int32) for b in blocks])
    s = dot(q_all, keys, ((1,), (1,))) * ((NOPE + ROPE) ** (-0.5))
    visible = key_positions[None, None, :] <= positions[None, :, None]
    s = jnp.where(visible, s.reshape(mla_local, rows, -1), -jnp.inf).reshape(mla_local * rows, -1)
    top = jnp.max(s, axis=-1, keepdims=True)
    e = jnp.exp(s - top)
    total = jnp.sum(e, axis=-1, keepdims=True)
    weighted = dot(e.astype(BF16), keys[:, :KVR])
    log_weight = (top + jnp.log(total))[:, 0].reshape(1, mla_local, rows)
    mean = (weighted / total).astype(BF16)
    mla_heads = jnp.concatenate(
        [
            dot(mean[h * rows : (h + 1) * rows], up_values[:, h * VDM : (h + 1) * VDM]).astype(BF16)
            for h in range(mla_local)
        ],
        axis=-1,
    )

    for h in range(ret_local):
        cross = dot(rq[h], carried[h].astype(BF16)) * (scale * jnp.exp(cumulative[h])[:, None])
        retained = intra[h] + cross
        norm = lax.rsqrt(jnp.mean(retained * retained, axis=-1, keepdims=True) + 1e-06)
        ret_heads.append((retained * norm * ret_gain[h * VD : (h + 1) * VD]).astype(BF16))
    ret_heads = jnp.concatenate(ret_heads, axis=-1)

    if fs_size == 2:
        near = dot(ret_heads, ret_out) + dot(mla_heads, mla_out)
        far = dot(ret_heads, far_ret) + dot(mla_heads, far_mla)
        first = lax.axis_index("fs") == 0
        partial = jnp.concatenate([jnp.where(first, near, far), jnp.where(first, far, near)], axis=1).astype(BF16)
    else:
        partial = (dot(ret_heads, far_ret) + dot(mla_heads, far_mla)).astype(BF16)
    tp_size = lax.axis_size("tp")
    if tp_size == 2:
        half = rows // 2
        mine = lax.dynamic_slice_in_dim(partial, core * half, half, 0)
        theirs = lax.dynamic_slice_in_dim(partial, (1 - core) * half, half, 0)
        mixed = (mine.astype(F32) + swap(theirs, "tp", 1).astype(F32)).astype(BF16)
    else:
        mixed = lax.psum_scatter(partial, "tp", scatter_dimension=0, tiled=True)
    return mixed[:, None, :], log_weight


def solution(mesh):
    in_specs = (
        P("sp", "fs", "tp"),
        P("sp", "fs", "tp"),
        P("sp", "fs", "tp"),
        P("fs", "tp", "sp"),
        P("tp"),
        P("sp", "fs", "tp"),
        P("sp", "fs", None),
        P("sp", "fs", None),
        P(),
        P(),
        P("tp", "fs"),
        P("tp", "fs"),
    )
    out_specs = (P(("sp", "tp"), "fs", None), P("fs", "tp", "sp"))
    return jax.shard_map(on_device, mesh=mesh, in_specs=in_specs, out_specs=out_specs, check_vma=False)
```

```python
import jax
import jax.numpy as jnp
from jax import lax
from jax.experimental import pallas as pl
from jax.experimental.pallas import tpu as pltpu
from jax.sharding import PartitionSpec as P

QK = 128
VD = 256
NOPE = 128
ROPE = 64
VDM = 128
KVR = 256
F32 = jnp.float32
BF16 = jnp.bfloat16


def swap(x, axis, distance):
    size = lax.axis_size(axis)
    return lax.ppermute(x, axis, [(i, i ^ distance) for i in range(size)])


def angles_of(positions, half_width):
    inverse = 1.0 / 10000.0 ** (jnp.arange(half_width, dtype=F32) / half_width)
    angles = positions.astype(F32)[:, None] * inverse[None, :]
    return jnp.cos(angles), jnp.sin(angles)


def rotate(vectors, cosine, sine):
    half_width = vectors.shape[-1] // 2
    wide = vectors.astype(F32)
    front, back = wide[..., :half_width], wide[..., half_width:]
    return jnp.concatenate([front * cosine - back * sine, front * sine + back * cosine], axis=-1).astype(BF16)


def dot(a, b, dims=((1,), (0,))):
    return lax.dot_general(a, b, (dims, ((), ())), preferred_element_type=F32)


def gather_keys(own):
    n = lax.axis_size("sp")
    place = lax.axis_index("sp")
    if n != 8 or lax.axis_size("tp") != 2:
        every = lax.all_gather(own, "sp", axis=0, tiled=False)
        return list(every), [jnp.int32(j) for j in range(n)]
    core = lax.axis_index("tp")
    got = []
    for step in (1, 3, 5):
        perm = [(2 * i + t, 2 * (i ^ (step + t)) + t) for i in range(n) for t in range(2)]
        got.append(lax.ppermute(own, ("sp", "tp"), perm))
    last = swap(own, "sp", 7)
    other = swap(jnp.concatenate(got, axis=0), "tp", 1)
    rows = own.shape[0]
    pieces = [own, last] + got + [other[rows * k : rows * (k + 1)] for k in range(3)]
    steps = [jnp.int32(0), jnp.int32(7)] + [s + core for s in (1, 3, 5)] + [s + 1 - core for s in (1, 3, 5)]
    return pieces, [place ^ s for s in steps]


def entering_state(state, log_total):
    n = lax.axis_size("sp")
    place = lax.axis_index("sp")
    heads = state.shape[0]
    total, total_log = state, log_total
    before = jnp.zeros_like(state)
    before_log = jnp.zeros_like(log_total)
    distance = 1
    while distance < n:
        high = lax.reduce_precision(total_log, 8, 7)
        pair = jnp.stack([high, total_log - high], axis=0)
        tail = jnp.broadcast_to(jnp.pad(pair, ((0, 6), (0, 0)))[:, :, None], (8, heads, VD // heads)).reshape(8, VD)
        message = jnp.concatenate([total.astype(BF16).reshape(heads * QK, VD), tail.astype(BF16)], axis=0)
        seen = swap(message, "sp", distance)
        seen_total = seen[: heads * QK].astype(F32).reshape(heads, QK, VD)
        logs = seen[heads * QK : heads * QK + 2].astype(F32)
        seen_log = jnp.sum(logs, axis=0)[:: VD // heads]
        upper = (place & distance) != 0
        before = jnp.where(upper, before + jnp.exp(before_log)[:, None, None] * seen_total, before)
        before_log = jnp.where(upper, before_log + seen_log, before_log)
        if 2 * distance < n:
            early = jnp.where(upper, seen_total, total)
            late = jnp.where(upper, total, seen_total)
            late_log = jnp.where(upper, total_log, seen_log)
            total = jnp.exp(late_log)[:, None, None] * early + late
            total_log = total_log + seen_log
        distance *= 2
    return before


def call(body, outs, args, flops=2_000_000, scratch=()):
    specs = [
        pl.BlockSpec(memory_space=pltpu.SMEM if a.dtype == jnp.int32 else pltpu.VMEM) for a in args
    ]
    shapes = [jax.ShapeDtypeStruct(shape, kind) for shape, kind in outs]
    return pl.pallas_call(
        body,
        out_shape=shapes,
        in_specs=specs,
        out_specs=[pl.BlockSpec(memory_space=pltpu.VMEM) for _ in shapes],
        scratch_shapes=list(scratch),
        cost_estimate=pl.CostEstimate(flops=flops, bytes_accessed=1_000_000, transcendentals=0),
    )(*args)


def turn(wide, cosine, sine):
    half = wide.shape[-1] // 2
    front, back = wide[:, :half], wide[:, half:]
    return jnp.concatenate([front * cosine - back * sine, front * sine + back * cosine], axis=-1)


def pack_body(place, inverse, latent, rope, own, cosine, sine):
    rows = latent.shape[0]
    at = place[0] * rows + lax.broadcasted_iota(jnp.int32, (rows, 128), 0)
    angle = at.astype(F32) * inverse[...]
    cos_all, sin_all = jnp.cos(angle), jnp.sin(angle)
    cosine[...] = cos_all
    sine[...] = sin_all
    half = ROPE // 2
    turned = turn(rope[...].astype(F32), cos_all[:, 64 : 64 + half], sin_all[:, 64 : 64 + half])
    own[:, :KVR] = latent[...]
    own[:, KVR:] = jnp.concatenate([turned, jnp.zeros((rows, 128 - ROPE), F32)], axis=-1).astype(BF16)


def message_of(message, total, logs):
    size = total.shape[0]
    message[:size, :] = total.astype(BF16)
    high = logs.astype(BF16).astype(F32)
    row = lax.broadcasted_iota(jnp.int32, logs.shape, 0)
    message[size:, :] = jnp.where(row == 0, high, logs - high).astype(BF16)


def state_body(query, key, value, decay, cos, sin, rq, rk, col, line, total, total_log, message):
    rows = query.shape[0]
    heads = decay.shape[0]
    first = lax.broadcasted_iota(jnp.int32, (rows, rows), 0)
    second = lax.broadcasted_iota(jnp.int32, (rows, rows), 1)
    lower = (second <= first).astype(F32)
    upper = (first <= second).astype(F32)
    high = lax.Precision.HIGHEST
    padded = jnp.concatenate([decay[...], jnp.zeros((8 - heads, rows), F32)], axis=0)
    sums = lax.dot_general(padded, upper, (((1,), (0,)), ((), ())), precision=high, preferred_element_type=F32)
    down = lax.dot_general(lower, padded, (((1,), (1,)), ((), ())), precision=high, preferred_element_type=F32)
    line[...] = sums
    col[...] = down
    cosine, sine = cos[:, :64], sin[:, :64]
    logs = []
    states = []
    for h in range(heads):
        part = slice(h * QK, (h + 1) * QK)
        rq[:, part] = turn(query[:, part].astype(F32), cosine, sine).astype(BF16)
        turned = turn(key[:, part].astype(F32), cosine, sine).astype(BF16)
        rk[:, part] = turned
        end = down[rows - 1 : rows, h : h + 1]
        faded = (turned.astype(F32) * jnp.exp(end - down[:, h : h + 1])).astype(BF16)
        states.append(dot(faded, value[:, h * VD : (h + 1) * VD], ((0,), (0,))))
        logs.append(jnp.broadcast_to(end, (16, VD // heads)))
    state = jnp.concatenate(states, axis=0)
    log = jnp.concatenate(logs, axis=1)
    total[...] = state
    total_log[...] = log
    message_of(message, state, log)


def fade(logs, heads):
    lanes = VD // heads
    return jnp.concatenate(
        [jnp.broadcast_to(jnp.exp(logs[0:1, h * lanes : h * lanes + 1]), (QK, VD)) for h in range(heads)], axis=0
    )


def opened(seen, heads):
    size = heads * QK
    pieces = seen[size:, :].astype(F32)
    both = pieces[0:1, :] + pieces[1:2, :]
    return seen[:size, :].astype(F32), jnp.broadcast_to(both, (16, VD))


def round_body(upper, seen, total, total_log, before, before_log, message, total_o, log_o, before_o, before_log_o):
    heads = total.shape[0] // QK
    other, other_log = opened(seen, heads)
    up = upper[0].astype(F32)
    before_o[...] = before[...] + up * fade(before_log[...], heads) * other
    before_log_o[...] = before_log[...] + up * other_log
    mine, mine_log = total[...], total_log[...]
    early = up * other + (1.0 - up) * mine
    late = up * mine + (1.0 - up) * other
    late_log = up * mine_log + (1.0 - up) * other_log
    fresh = fade(late_log, heads) * early + late
    fresh_log = mine_log + other_log
    total_o[...] = fresh
    log_o[...] = fresh_log
    message_of(message, fresh, fresh_log)


def query_body(core, rq, rk, value, col, line, query, key_up, cos, sin, intra, q_all):
    rows = rq.shape[0]
    heads = rq.shape[1] // QK
    first = lax.broadcasted_iota(jnp.int32, (rows, rows), 0)
    second = lax.broadcasted_iota(jnp.int32, (rows, rows), 1)
    causal = second <= first
    for h in range(heads):
        part = slice(h * QK, (h + 1) * QK)
        gap = col[:, h : h + 1] - line[h : h + 1, :]
        score = dot(rq[:, part], rk[:, part], ((1,), (1,))) * QK ** (-0.5)
        weight = jnp.where(causal, score * jnp.exp(jnp.where(causal, gap, 0.0)), 0.0).astype(BF16)
        intra[:, h * VD : (h + 1) * VD] = dot(weight, value[:, h * VD : (h + 1) * VD])
    width = NOPE + ROPE
    local = query.shape[1] // width
    half = ROPE // 2
    cosine, sine = cos[:, 64 : 64 + half], sin[:, 64 : 64 + half]
    begin = core[0] * (local * NOPE)
    for h in range(local):
        one = query[:, h * width : (h + 1) * width]
        up = key_up[:, pl.ds(pl.multiple_of(begin + h * NOPE, 128), NOPE)]
        q_all[h * rows : (h + 1) * rows, :KVR] = dot(one[:, :NOPE], up, ((1,), (1,))).astype(BF16)
        turned = turn(one[:, NOPE:].astype(F32), cosine, sine)
        wide = jnp.concatenate([turned, jnp.zeros((rows, 128 - ROPE), F32)], axis=-1)
        q_all[h * rows : (h + 1) * rows, KVR:] = wide.astype(BF16)


def attend_body(seat, q_all, value_up, *rest):
    count = len(rest) - 3
    keys = rest[:count]
    heads_o, logs_o, scores = rest[count:]
    rows = keys[0].shape[0]
    local = q_all.shape[0] // rows
    scale = (NOPE + ROPE) ** (-0.5)
    q = q_all[...]
    at = lax.broadcasted_iota(jnp.int32, (q.shape[0], rows), 0) % rows
    tops = []
    for b in range(count):
        s = dot(q, keys[b][...], ((1,), (1,))) * scale
        if b == 0:
            s = jnp.where(lax.broadcasted_iota(jnp.int32, s.shape, 1) <= at, s, -jnp.inf)
        else:
            s = jnp.where(seat[1 + b] < seat[0], s, -jnp.inf)
        scores[b] = s
        tops.append(s)
    while len(tops) > 1:
        tops = [jnp.maximum(tops[k], tops[k + 1]) if k + 1 < len(tops) else tops[k] for k in range(0, len(tops), 2)]
    top = jnp.max(tops[0], axis=-1, keepdims=True)
    sums = jnp.zeros((q.shape[0], rows), F32)
    weighted = jnp.zeros((q.shape[0], KVR), F32)
    for b in range(count):
        e = jnp.exp(scores[b] - top)
        sums = sums + e
        weighted = weighted + dot(e.astype(BF16), keys[b][:, :KVR])
    total = jnp.sum(sums, axis=-1, keepdims=True)
    log = top + jnp.log(total)
    mean = (weighted / total).astype(BF16)
    begin = seat[1] * (local * VDM)
    for h in range(local):
        part = slice(h * rows, (h + 1) * rows)
        up = value_up[:, pl.ds(pl.multiple_of(begin + h * VDM, 128), VDM)]
        heads_o[:, h * VDM : (h + 1) * VDM] = dot(mean[part], up).astype(BF16)
        logs_o[h : h + 1, :] = jnp.broadcast_to(log[part], (rows, rows)).T[0:1, :]


def heads_body(upper, seen, before, before_log, rq, col, intra, gain, mla_heads, ret_w, mla_w, ret_heads, near):
    heads = rq.shape[1] // QK
    other, _ = opened(seen, heads)
    carried = before[...] + upper[0].astype(F32) * fade(before_log[...], heads) * other
    carried = carried.astype(BF16)
    for h in range(heads):
        part = slice(h * VD, (h + 1) * VD)
        cross = dot(rq[:, h * QK : (h + 1) * QK], carried[h * QK : (h + 1) * QK])
        retained = intra[:, part] + cross * (QK ** (-0.5) * jnp.exp(col[:, h : h + 1]))
        norm = lax.rsqrt(jnp.mean(retained * retained, axis=-1, keepdims=True) + 1e-06)
        ret_heads[:, part] = (retained * norm * gain[:, part]).astype(BF16)
    near[...] = (dot(ret_heads[...], ret_w[...]) + dot(mla_heads[...], mla_w[...])).astype(BF16)


def merge_body(seat, near, ret_heads, mla_heads, ret_w, mla_w, mine, theirs):
    width = near.shape[1]
    half = mine.shape[0]
    far = (dot(ret_heads[...], ret_w[...]) + dot(mla_heads[...], mla_w[...])).astype(BF16)
    upper, lower = far[half:], far[:half]
    here = pl.ds(pl.multiple_of(seat[1] * width, 128), width)
    there = pl.ds(pl.multiple_of((1 - seat[1]) * width, 128), width)
    first = seat[0] == 0
    mine[:, there] = jnp.where(first, lower, upper)
    theirs[:, there] = jnp.where(first, upper, lower)
    mine[:, here] = jnp.where(first, near[:half, :], near[half:, :])
    theirs[:, here] = jnp.where(first, near[half:, :], near[:half, :])


def one(value):
    return jnp.asarray(value, jnp.int32).reshape(1)


def with_kernels(
    ret_query, ret_key, ret_value, log_decay, ret_gain, mla_query,
    kv_latent, rope_key, key_up, value_up, ret_out, mla_out,
):
    rows = ret_query.shape[0]
    heads = ret_value.shape[2] // VD
    local = mla_query.shape[2] // (NOPE + ROPE)
    core, place, side = (lax.axis_index(a) for a in ("tp", "sp", "fs"))
    n = lax.axis_size("sp")
    columns = ret_out.shape[1]
    far_ret = swap(ret_out, "fs", 1)
    far_mla = swap(mla_out, "fs", 1)
    lane = jnp.arange(128)
    power = jnp.where(lane < 64, lane / 64.0, (lane - 64) / 32.0).astype(F32)
    inverse = (1.0 / 10000.0**power)[None]
    own, cos, sin = call(
        pack_body,
        [((rows, 384), BF16), ((rows, 128), F32), ((rows, 128), F32)],
        [one(place), inverse, kv_latent[:, 0], rope_key[:, 0]],
    )
    got = []
    for step in (1, 3, 5):
        perm = [(2 * i + t, 2 * (i ^ (step + t)) + t) for i in range(n) for t in range(2)]
        got.append(lax.ppermute(own, ("sp", "tp"), perm))
    last = swap(own, "sp", 7)
    big = heads * QK
    wide = [((big + 16, VD), BF16), ((big, VD), F32), ((16, VD), F32), ((big, VD), F32), ((16, VD), F32)]
    rq, rk, col, line, total, total_log, message = call(
        state_body,
        [((rows, big), BF16), ((rows, big), BF16), ((rows, 8), F32), ((8, rows), F32), wide[1], wide[2], wide[0]],
        [ret_query[:, 0], ret_key[:, 0], ret_value[:, 0], log_decay[0], cos, sin],
    )
    before, before_log = jnp.zeros((big, VD), F32), jnp.zeros((16, VD), F32)
    distance = 1
    while distance < n:
        seen = swap(message, "sp", distance)
        upper = one((place // distance) % 2)
        if 2 * distance < n:
            message, total, total_log, before, before_log = call(
                round_body, wide, [upper, seen, total, total_log, before, before_log]
            )
        distance *= 2
    intra, q_all = call(
        query_body,
        [((rows, heads * VD), F32), ((local * rows, 384), BF16)],
        [one(core), rq, rk, ret_value[:, 0], col, line, mla_query[:, 0], key_up, cos, sin],
        flops=8_000_000,
    )
    other = [swap(g, "tp", 1) for g in got]
    steps = [0, 7] + [s + core for s in (1, 3, 5)] + [s + 1 - core for s in (1, 3, 5)]
    seat = jnp.stack([jnp.asarray(v, jnp.int32) for v in [place, core] + [place ^ s for s in steps[1:]]])
    keys = [own, last] + got + other
    mla_heads, logs = call(
        attend_body,
        [((rows, local * VDM), BF16), ((local, rows), F32)],
        [seat, q_all, value_up] + keys,
        flops=12_000_000,
        scratch=[pltpu.VMEM((len(keys), local * rows, rows), F32)],
    )
    ret_heads, near = call(
        heads_body,
        [((rows, heads * VD), BF16), ((rows, columns), BF16)],
        [upper, seen, before, before_log, rq, col, intra, ret_gain[None], mla_heads, ret_out, mla_out],
    )
    mine, theirs = call(
        merge_body,
        [((rows // 2, 2 * columns), BF16), ((rows // 2, 2 * columns), BF16)],
        [jnp.stack([core, side]).astype(jnp.int32), near, ret_heads, mla_heads, far_ret, far_mla],
    )
    mixed = (mine.astype(F32) + swap(theirs, "tp", 1).astype(F32)).astype(BF16)
    return mixed[:, None, :], logs[None]


def on_device(
    ret_query, ret_key, ret_value, log_decay, ret_gain, mla_query,
    kv_latent, rope_key, key_up, value_up, ret_out, mla_out,
):
    rows = ret_query.shape[0]
    ret_local = ret_value.shape[2] // VD
    mla_local = mla_query.shape[2] // (NOPE + ROPE)
    core = lax.axis_index("tp")
    place = lax.axis_index("sp")
    fs_size = lax.axis_size("fs")
    positions = place * rows + jnp.arange(rows, dtype=jnp.int32)
    if fs_size == 2:
        far_ret, far_mla = swap(ret_out, "fs", 1), swap(mla_out, "fs", 1)
    else:
        far_ret = lax.all_gather(ret_out, "fs", axis=1, tiled=True)
        far_mla = lax.all_gather(mla_out, "fs", axis=1, tiled=True)

    cos_a, sin_a = angles_of(positions, ROPE // 2)
    own_rope = rotate(rope_key[:, 0], cos_a, sin_a)
    own = jnp.concatenate([kv_latent[:, 0], own_rope, jnp.zeros((rows, 128 - ROPE), BF16)], axis=-1)
    pieces, blocks = gather_keys(own)

    cos_r, sin_r = angles_of(positions, QK // 2)
    cumulative = jnp.cumsum(log_decay[0], axis=-1)
    rq = [rotate(ret_query[:, 0, h * QK : (h + 1) * QK], cos_r, sin_r) for h in range(ret_local)]
    rk = [rotate(ret_key[:, 0, h * QK : (h + 1) * QK], cos_r, sin_r) for h in range(ret_local)]
    rv = [ret_value[:, 0, h * VD : (h + 1) * VD] for h in range(ret_local)]
    tail = jnp.exp(cumulative[:, -1:] - cumulative)
    state = jnp.stack(
        [dot((rk[h].astype(F32) * tail[h][:, None]).astype(BF16), rv[h], ((0,), (0,))) for h in range(ret_local)]
    )
    carried = entering_state(state, cumulative[:, -1])

    scale = QK ** (-0.5)
    causal = jnp.tril(jnp.ones((rows, rows), dtype=bool))
    ret_heads = []
    intra = []
    for h in range(ret_local):
        gap = cumulative[h][:, None] - cumulative[h][None, :]
        score = dot(rq[h], rk[h], ((1,), (1,))) * scale
        weight = jnp.where(causal, score * jnp.exp(jnp.where(causal, gap, 0.0)), 0.0).astype(BF16)
        intra.append(dot(weight, rv[h]))

    head_rows = mla_query[:, 0].reshape(rows, mla_local, NOPE + ROPE)
    up_keys = lax.dynamic_slice_in_dim(key_up, core * (mla_local * NOPE), mla_local * NOPE, 1)
    up_values = lax.dynamic_slice_in_dim(value_up, core * (mla_local * VDM), mla_local * VDM, 1)
    q_parts = []
    for h in range(mla_local):
        absorbed = dot(head_rows[:, h, :NOPE], up_keys[:, h * NOPE : (h + 1) * NOPE], ((1,), (1,))).astype(BF16)
        aq = rotate(head_rows[:, h, NOPE:], cos_a, sin_a)
        q_parts.append(jnp.concatenate([absorbed, aq, jnp.zeros((rows, 128 - ROPE), BF16)], axis=-1))
    q_all = jnp.concatenate(q_parts, axis=0)
    keys = jnp.concatenate(pieces, axis=0)
    key_positions = jnp.concatenate([b * rows + jnp.arange(rows, dtype=jnp.int32) for b in blocks])
    s = dot(q_all, keys, ((1,), (1,))) * ((NOPE + ROPE) ** (-0.5))
    visible = key_positions[None, None, :] <= positions[None, :, None]
    s = jnp.where(visible, s.reshape(mla_local, rows, -1), -jnp.inf).reshape(mla_local * rows, -1)
    top = jnp.max(s, axis=-1, keepdims=True)
    e = jnp.exp(s - top)
    total = jnp.sum(e, axis=-1, keepdims=True)
    weighted = dot(e.astype(BF16), keys[:, :KVR])
    log_weight = (top + jnp.log(total))[:, 0].reshape(1, mla_local, rows)
    mean = (weighted / total).astype(BF16)
    mla_heads = jnp.concatenate(
        [
            dot(mean[h * rows : (h + 1) * rows], up_values[:, h * VDM : (h + 1) * VDM]).astype(BF16)
            for h in range(mla_local)
        ],
        axis=-1,
    )

    for h in range(ret_local):
        cross = dot(rq[h], carried[h].astype(BF16)) * (scale * jnp.exp(cumulative[h])[:, None])
        retained = intra[h] + cross
        norm = lax.rsqrt(jnp.mean(retained * retained, axis=-1, keepdims=True) + 1e-06)
        ret_heads.append((retained * norm * ret_gain[h * VD : (h + 1) * VD]).astype(BF16))
    ret_heads = jnp.concatenate(ret_heads, axis=-1)

    if fs_size == 2:
        near = dot(ret_heads, ret_out) + dot(mla_heads, mla_out)
        far = dot(ret_heads, far_ret) + dot(mla_heads, far_mla)
        first = lax.axis_index("fs") == 0
        partial = jnp.concatenate([jnp.where(first, near, far), jnp.where(first, far, near)], axis=1).astype(BF16)
    else:
        partial = (dot(ret_heads, far_ret) + dot(mla_heads, far_mla)).astype(BF16)
    tp_size = lax.axis_size("tp")
    if tp_size == 2:
        half = rows // 2
        mine = lax.dynamic_slice_in_dim(partial, core * half, half, 0)
        theirs = lax.dynamic_slice_in_dim(partial, (1 - core) * half, half, 0)
        mixed = (mine.astype(F32) + swap(theirs, "tp", 1).astype(F32)).astype(BF16)
    else:
        mixed = lax.psum_scatter(partial, "tp", scatter_dimension=0, tiled=True)
    return mixed[:, None, :], log_weight


def solution(mesh):
    in_specs = (
        P("sp", "fs", "tp"),
        P("sp", "fs", "tp"),
        P("sp", "fs", "tp"),
        P("fs", "tp", "sp"),
        P("tp"),
        P("sp", "fs", "tp"),
        P("sp", "fs", None),
        P("sp", "fs", None),
        P(),
        P(),
        P("tp", "fs"),
        P("tp", "fs"),
    )
    out_specs = (P(("sp", "tp"), "fs", None), P("fs", "tp", "sp"))
    small = mesh.shape["sp"] == 8 and mesh.shape["fs"] == 2 and mesh.shape["tp"] == 2
    body = with_kernels if small else on_device
    return jax.shard_map(body, mesh=mesh, in_specs=in_specs, out_specs=out_specs, check_vma=False)
```

```python
import jax
import jax.numpy as jnp
from jax import lax
from jax.experimental import pallas as pl
from jax.experimental.pallas import tpu as pltpu
from jax.sharding import PartitionSpec as P

QK = 128
VD = 256
NOPE = 128
ROPE = 64
VDM = 128
KVR = 256
F32 = jnp.float32
BF16 = jnp.bfloat16


def swap(x, axis, distance):
    size = lax.axis_size(axis)
    return lax.ppermute(x, axis, [(i, i ^ distance) for i in range(size)])


def angles_of(positions, half_width):
    inverse = 1.0 / 10000.0 ** (jnp.arange(half_width, dtype=F32) / half_width)
    angles = positions.astype(F32)[:, None] * inverse[None, :]
    return jnp.cos(angles), jnp.sin(angles)


def rotate(vectors, cosine, sine):
    half_width = vectors.shape[-1] // 2
    wide = vectors.astype(F32)
    front, back = wide[..., :half_width], wide[..., half_width:]
    return jnp.concatenate([front * cosine - back * sine, front * sine + back * cosine], axis=-1).astype(BF16)


def dot(a, b, dims=((1,), (0,))):
    return lax.dot_general(a, b, (dims, ((), ())), preferred_element_type=F32)


def gather_keys(own):
    n = lax.axis_size("sp")
    place = lax.axis_index("sp")
    if n != 8 or lax.axis_size("tp") != 2:
        every = lax.all_gather(own, "sp", axis=0, tiled=False)
        return list(every), [jnp.int32(j) for j in range(n)]
    core = lax.axis_index("tp")
    got = []
    for step in (1, 3, 5):
        perm = [(2 * i + t, 2 * (i ^ (step + t)) + t) for i in range(n) for t in range(2)]
        got.append(lax.ppermute(own, ("sp", "tp"), perm))
    last = swap(own, "sp", 7)
    other = swap(jnp.concatenate(got, axis=0), "tp", 1)
    rows = own.shape[0]
    pieces = [own, last] + got + [other[rows * k : rows * (k + 1)] for k in range(3)]
    steps = [jnp.int32(0), jnp.int32(7)] + [s + core for s in (1, 3, 5)] + [s + 1 - core for s in (1, 3, 5)]
    return pieces, [place ^ s for s in steps]


def entering_state(state, log_total):
    n = lax.axis_size("sp")
    place = lax.axis_index("sp")
    heads = state.shape[0]
    total, total_log = state, log_total
    before = jnp.zeros_like(state)
    before_log = jnp.zeros_like(log_total)
    distance = 1
    while distance < n:
        high = lax.reduce_precision(total_log, 8, 7)
        pair = jnp.stack([high, total_log - high], axis=0)
        tail = jnp.broadcast_to(jnp.pad(pair, ((0, 6), (0, 0)))[:, :, None], (8, heads, VD // heads)).reshape(8, VD)
        message = jnp.concatenate([total.astype(BF16).reshape(heads * QK, VD), tail.astype(BF16)], axis=0)
        seen = swap(message, "sp", distance)
        seen_total = seen[: heads * QK].astype(F32).reshape(heads, QK, VD)
        logs = seen[heads * QK : heads * QK + 2].astype(F32)
        seen_log = jnp.sum(logs, axis=0)[:: VD // heads]
        upper = (place & distance) != 0
        before = jnp.where(upper, before + jnp.exp(before_log)[:, None, None] * seen_total, before)
        before_log = jnp.where(upper, before_log + seen_log, before_log)
        if 2 * distance < n:
            early = jnp.where(upper, seen_total, total)
            late = jnp.where(upper, total, seen_total)
            late_log = jnp.where(upper, total_log, seen_log)
            total = jnp.exp(late_log)[:, None, None] * early + late
            total_log = total_log + seen_log
        distance *= 2
    return before


def call(body, outs, args, flops=2_000_000, scratch=()):
    specs = [
        pl.BlockSpec(memory_space=pltpu.SMEM if a.dtype == jnp.int32 else pltpu.VMEM) for a in args
    ]
    shapes = [pltpu.VMEM(shape, kind) for shape, kind in outs]
    args = [a if a.dtype == jnp.int32 else pltpu.with_memory_space_constraint(a, pltpu.VMEM) for a in args]
    return pl.pallas_call(
        body,
        out_shape=shapes,
        in_specs=specs,
        out_specs=[pl.BlockSpec(memory_space=pltpu.VMEM) for _ in shapes],
        scratch_shapes=list(scratch),
        compiler_params=pltpu.CompilerParams(vmem_limit_bytes=16 * 1024 * 1024),
        cost_estimate=pl.CostEstimate(flops=flops, bytes_accessed=1_000_000, transcendentals=0),
    )(*args)


def turn(wide, cosine, sine):
    half = wide.shape[-1] // 2
    front, back = wide[:, :half], wide[:, half:]
    return jnp.concatenate([front * cosine - back * sine, front * sine + back * cosine], axis=-1)


def pack_body(place, inverse, latent, rope, own, cosine, sine):
    rows = latent.shape[0]
    at = place[0] * rows + lax.broadcasted_iota(jnp.int32, (rows, 128), 0)
    angle = at.astype(F32) * inverse[...]
    cos_all, sin_all = jnp.cos(angle), jnp.sin(angle)
    cosine[...] = cos_all
    sine[...] = sin_all
    half = ROPE // 2
    turned = turn(rope[...].astype(F32), cos_all[:, 64 : 64 + half], sin_all[:, 64 : 64 + half])
    own[:, :KVR] = latent[...]
    own[:, KVR:] = jnp.concatenate([turned, jnp.zeros((rows, 128 - ROPE), F32)], axis=-1).astype(BF16)


def message_of(message, total, logs):
    size = total.shape[0]
    message[:size, :] = total.astype(BF16)
    high = logs.astype(BF16).astype(F32)
    row = lax.broadcasted_iota(jnp.int32, logs.shape, 0)
    message[size:, :] = jnp.where(row == 0, high, logs - high).astype(BF16)


def state_body(query, key, value, decay, cos, sin, rq, rk, col, line, total, total_log, message):
    rows = query.shape[0]
    heads = decay.shape[0]
    first = lax.broadcasted_iota(jnp.int32, (rows, rows), 0)
    second = lax.broadcasted_iota(jnp.int32, (rows, rows), 1)
    lower = (second <= first).astype(F32)
    upper = (first <= second).astype(F32)
    high = lax.Precision.HIGHEST
    padded = jnp.concatenate([decay[...], jnp.zeros((8 - heads, rows), F32)], axis=0)
    sums = lax.dot_general(padded, upper, (((1,), (0,)), ((), ())), precision=high, preferred_element_type=F32)
    down = lax.dot_general(lower, padded, (((1,), (1,)), ((), ())), precision=high, preferred_element_type=F32)
    line[...] = sums
    col[...] = down
    cosine, sine = cos[:, :64], sin[:, :64]
    logs = []
    states = []
    for h in range(heads):
        part = slice(h * QK, (h + 1) * QK)
        rq[:, part] = turn(query[:, part].astype(F32), cosine, sine).astype(BF16)
        turned = turn(key[:, part].astype(F32), cosine, sine).astype(BF16)
        rk[:, part] = turned
        end = down[rows - 1 : rows, h : h + 1]
        faded = (turned.astype(F32) * jnp.exp(end - down[:, h : h + 1])).astype(BF16)
        states.append(dot(faded, value[:, h * VD : (h + 1) * VD], ((0,), (0,))))
        logs.append(jnp.broadcast_to(end, (16, VD // heads)))
    state = jnp.concatenate(states, axis=0)
    log = jnp.concatenate(logs, axis=1)
    total[...] = state
    total_log[...] = log
    message_of(message, state, log)


def fade(logs, heads):
    lanes = VD // heads
    return jnp.concatenate(
        [jnp.broadcast_to(jnp.exp(logs[0:1, h * lanes : h * lanes + 1]), (QK, VD)) for h in range(heads)], axis=0
    )


def opened(seen, heads):
    size = heads * QK
    pieces = seen[size:, :].astype(F32)
    both = pieces[0:1, :] + pieces[1:2, :]
    return seen[:size, :].astype(F32), jnp.broadcast_to(both, (16, VD))


def round_body(upper, seen, total, total_log, before, before_log, message, total_o, log_o, before_o, before_log_o):
    heads = total.shape[0] // QK
    other, other_log = opened(seen, heads)
    up = upper[0].astype(F32)
    if before is None:
        before_o[...] = up * other
        before_log_o[...] = up * other_log
    else:
        before_o[...] = before[...] + up * fade(before_log[...], heads) * other
        before_log_o[...] = before_log[...] + up * other_log
    mine, mine_log = total[...], total_log[...]
    early = up * other + (1.0 - up) * mine
    late = up * mine + (1.0 - up) * other
    late_log = up * mine_log + (1.0 - up) * other_log
    fresh = fade(late_log, heads) * early + late
    fresh_log = mine_log + other_log
    total_o[...] = fresh
    log_o[...] = fresh_log
    message_of(message, fresh, fresh_log)


def first_body(upper, seen, total, total_log, message, total_o, log_o, before_o, before_log_o):
    round_body(upper, seen, total, total_log, None, None, message, total_o, log_o, before_o, before_log_o)


def query_body(core, rq, rk, value, col, line, query, key_up, cos, sin, intra, q_all):
    rows = rq.shape[0]
    heads = rq.shape[1] // QK
    first = lax.broadcasted_iota(jnp.int32, (rows, rows), 0)
    second = lax.broadcasted_iota(jnp.int32, (rows, rows), 1)
    causal = second <= first
    for h in range(heads):
        part = slice(h * QK, (h + 1) * QK)
        gap = col[:, h : h + 1] - line[h : h + 1, :]
        score = dot(rq[:, part], rk[:, part], ((1,), (1,))) * QK ** (-0.5)
        weight = jnp.where(causal, score * jnp.exp(jnp.where(causal, gap, 0.0)), 0.0).astype(BF16)
        intra[:, h * VD : (h + 1) * VD] = dot(weight, value[:, h * VD : (h + 1) * VD])
    width = NOPE + ROPE
    local = query.shape[1] // width
    half = ROPE // 2
    cosine, sine = cos[:, 64 : 64 + half], sin[:, 64 : 64 + half]
    begin = core[0] * (local * NOPE)
    for h in range(local):
        one = query[:, h * width : (h + 1) * width]
        up = key_up[:, pl.ds(pl.multiple_of(begin + h * NOPE, 128), NOPE)]
        q_all[h * rows : (h + 1) * rows, :KVR] = dot(one[:, :NOPE], up, ((1,), (1,))).astype(BF16)
        turned = turn(one[:, NOPE:].astype(F32), cosine, sine)
        wide = jnp.concatenate([turned, jnp.zeros((rows, 128 - ROPE), F32)], axis=-1)
        q_all[h * rows : (h + 1) * rows, KVR:] = wide.astype(BF16)


def attend_body(place, core, q_all, value_up, *rest):
    count = len(rest) - 3
    keys = rest[:count]
    heads_o, logs_o, scores = rest[count:]
    rows = keys[0].shape[0]
    local = q_all.shape[0] // rows
    scale = (NOPE + ROPE) ** (-0.5)
    q = q_all[...]
    at = lax.broadcasted_iota(jnp.int32, (q.shape[0], rows), 0) % rows
    tops = []
    t = core[0]
    steps = [0, 7] + [d + t for d in (1, 3, 5)] + [d + 1 - t for d in (1, 3, 5)]
    for b in range(count):
        s = dot(q, keys[b][...], ((1,), (1,))) * scale
        if b == 0:
            s = jnp.where(lax.broadcasted_iota(jnp.int32, s.shape, 1) <= at, s, -jnp.inf)
        else:
            s = jnp.where((place[0] ^ steps[b]) < place[0], s, -jnp.inf)
        scores[b] = s
        tops.append(s)
    while len(tops) > 1:
        tops = [jnp.maximum(tops[k], tops[k + 1]) if k + 1 < len(tops) else tops[k] for k in range(0, len(tops), 2)]
    top = jnp.max(tops[0], axis=-1, keepdims=True)
    sums = jnp.zeros((q.shape[0], rows), F32)
    weighted = jnp.zeros((q.shape[0], KVR), F32)
    for b in range(count):
        e = jnp.exp(scores[b] - top)
        sums = sums + e
        weighted = weighted + dot(e.astype(BF16), keys[b][:, :KVR])
    total = jnp.sum(sums, axis=-1, keepdims=True)
    log = top + jnp.log(total)
    mean = (weighted / total).astype(BF16)
    begin = core[0] * (local * VDM)
    for h in range(local):
        part = slice(h * rows, (h + 1) * rows)
        up = value_up[:, pl.ds(pl.multiple_of(begin + h * VDM, 128), VDM)]
        heads_o[:, h * VDM : (h + 1) * VDM] = dot(mean[part], up).astype(BF16)
        logs_o[h : h + 1, :] = jnp.broadcast_to(log[part], (rows, rows)).T[0:1, :]


def heads_body(upper, seen, before, before_log, rq, col, intra, gain, mla_heads, ret_w, mla_w, ret_heads, near):
    heads = rq.shape[1] // QK
    other, _ = opened(seen, heads)
    carried = before[...] + upper[0].astype(F32) * fade(before_log[...], heads) * other
    carried = carried.astype(BF16)
    for h in range(heads):
        part = slice(h * VD, (h + 1) * VD)
        cross = dot(rq[:, h * QK : (h + 1) * QK], carried[h * QK : (h + 1) * QK])
        retained = intra[:, part] + cross * (QK ** (-0.5) * jnp.exp(col[:, h : h + 1]))
        norm = lax.rsqrt(jnp.mean(retained * retained, axis=-1, keepdims=True) + 1e-06)
        ret_heads[:, part] = (retained * norm * gain[:, part]).astype(BF16)
    near[...] = (dot(ret_heads[...], ret_w[...]) + dot(mla_heads[...], mla_w[...])).astype(BF16)


def merge_body(core, side, near, ret_heads, mla_heads, ret_w, mla_w, mine, theirs):
    width = near.shape[1]
    half = mine.shape[0]
    far = (dot(ret_heads[...], ret_w[...]) + dot(mla_heads[...], mla_w[...])).astype(BF16)
    upper, lower = far[half:], far[:half]
    here = pl.ds(pl.multiple_of(side[0] * width, 128), width)
    there = pl.ds(pl.multiple_of((1 - side[0]) * width, 128), width)
    first = core[0] == 0
    mine[:, there] = jnp.where(first, lower, upper)
    theirs[:, there] = jnp.where(first, upper, lower)
    mine[:, here] = jnp.where(first, near[:half, :], near[half:, :])
    theirs[:, here] = jnp.where(first, near[half:, :], near[:half, :])


def one(value):
    return jnp.asarray(value, jnp.int32).reshape(1)


def with_kernels(
    ret_query, ret_key, ret_value, log_decay, ret_gain, mla_query,
    kv_latent, rope_key, key_up, value_up, ret_out, mla_out,
):
    rows = ret_query.shape[0]
    heads = ret_value.shape[2] // VD
    local = mla_query.shape[2] // (NOPE + ROPE)
    core, place, side = (lax.axis_index(a) for a in ("tp", "sp", "fs"))
    n = lax.axis_size("sp")
    columns = ret_out.shape[1]
    far_ret = swap(ret_out, "fs", 1)
    far_mla = swap(mla_out, "fs", 1)
    lane = jnp.arange(128)
    power = jnp.where(lane < 64, lane / 64.0, (lane - 64) / 32.0).astype(F32)
    inverse = (1.0 / 10000.0**power)[None]
    own, cos, sin = call(
        pack_body,
        [((rows, 384), BF16), ((rows, 128), F32), ((rows, 128), F32)],
        [one(place), inverse, kv_latent[:, 0], rope_key[:, 0]],
    )
    got = []
    for step in (1, 3, 5):
        perm = [(2 * i + t, 2 * (i ^ (step + t)) + t) for i in range(n) for t in range(2)]
        got.append(lax.ppermute(own, ("sp", "tp"), perm))
    last = swap(own, "sp", 7)
    big = heads * QK
    wide = [((big + 16, VD), BF16), ((big, VD), F32), ((16, VD), F32), ((big, VD), F32), ((16, VD), F32)]
    rq, rk, col, line, total, total_log, message = call(
        state_body,
        [((rows, big), BF16), ((rows, big), BF16), ((rows, 8), F32), ((8, rows), F32), wide[1], wide[2], wide[0]],
        [ret_query[:, 0], ret_key[:, 0], ret_value[:, 0], log_decay[0], cos, sin],
    )
    carry = []
    distance = 1
    while distance < n:
        seen = swap(message, "sp", distance)
        upper = one((place // distance) % 2)
        if 2 * distance < n:
            body = round_body if carry else first_body
            message, total, total_log, *carry = call(body, wide, [upper, seen, total, total_log] + carry)
        distance *= 2
    intra, q_all = call(
        query_body,
        [((rows, heads * VD), F32), ((local * rows, 384), BF16)],
        [one(core), rq, rk, ret_value[:, 0], col, line, mla_query[:, 0], key_up, cos, sin],
        flops=8_000_000,
    )
    other = [swap(g, "tp", 1) for g in got]
    keys = [own, last] + got + other
    mla_heads, logs = call(
        attend_body,
        [((rows, local * VDM), BF16), ((local, rows), F32)],
        [one(place), one(core), q_all, value_up] + keys,
        flops=12_000_000,
        scratch=[pltpu.VMEM((len(keys), local * rows, rows), F32)],
    )
    ret_heads, near = call(
        heads_body,
        [((rows, heads * VD), BF16), ((rows, columns), BF16)],
        [upper, seen] + carry + [rq, col, intra, ret_gain[None], mla_heads, ret_out, mla_out],
    )
    mine, theirs = call(
        merge_body,
        [((rows // 2, 2 * columns), BF16), ((rows // 2, 2 * columns), BF16)],
        [one(core), one(side), near, ret_heads, mla_heads, far_ret, far_mla],
    )
    mixed = (mine.astype(F32) + swap(theirs, "tp", 1).astype(F32)).astype(BF16)
    return mixed[:, None, :], logs[None]


def on_device(
    ret_query, ret_key, ret_value, log_decay, ret_gain, mla_query,
    kv_latent, rope_key, key_up, value_up, ret_out, mla_out,
):
    rows = ret_query.shape[0]
    ret_local = ret_value.shape[2] // VD
    mla_local = mla_query.shape[2] // (NOPE + ROPE)
    core = lax.axis_index("tp")
    place = lax.axis_index("sp")
    fs_size = lax.axis_size("fs")
    positions = place * rows + jnp.arange(rows, dtype=jnp.int32)
    if fs_size == 2:
        far_ret, far_mla = swap(ret_out, "fs", 1), swap(mla_out, "fs", 1)
    else:
        far_ret = lax.all_gather(ret_out, "fs", axis=1, tiled=True)
        far_mla = lax.all_gather(mla_out, "fs", axis=1, tiled=True)

    cos_a, sin_a = angles_of(positions, ROPE // 2)
    own_rope = rotate(rope_key[:, 0], cos_a, sin_a)
    own = jnp.concatenate([kv_latent[:, 0], own_rope, jnp.zeros((rows, 128 - ROPE), BF16)], axis=-1)
    pieces, blocks = gather_keys(own)

    cos_r, sin_r = angles_of(positions, QK // 2)
    cumulative = jnp.cumsum(log_decay[0], axis=-1)
    rq = [rotate(ret_query[:, 0, h * QK : (h + 1) * QK], cos_r, sin_r) for h in range(ret_local)]
    rk = [rotate(ret_key[:, 0, h * QK : (h + 1) * QK], cos_r, sin_r) for h in range(ret_local)]
    rv = [ret_value[:, 0, h * VD : (h + 1) * VD] for h in range(ret_local)]
    tail = jnp.exp(cumulative[:, -1:] - cumulative)
    state = jnp.stack(
        [dot((rk[h].astype(F32) * tail[h][:, None]).astype(BF16), rv[h], ((0,), (0,))) for h in range(ret_local)]
    )
    carried = entering_state(state, cumulative[:, -1])

    scale = QK ** (-0.5)
    causal = jnp.tril(jnp.ones((rows, rows), dtype=bool))
    ret_heads = []
    intra = []
    for h in range(ret_local):
        gap = cumulative[h][:, None] - cumulative[h][None, :]
        score = dot(rq[h], rk[h], ((1,), (1,))) * scale
        weight = jnp.where(causal, score * jnp.exp(jnp.where(causal, gap, 0.0)), 0.0).astype(BF16)
        intra.append(dot(weight, rv[h]))

    head_rows = mla_query[:, 0].reshape(rows, mla_local, NOPE + ROPE)
    up_keys = lax.dynamic_slice_in_dim(key_up, core * (mla_local * NOPE), mla_local * NOPE, 1)
    up_values = lax.dynamic_slice_in_dim(value_up, core * (mla_local * VDM), mla_local * VDM, 1)
    q_parts = []
    for h in range(mla_local):
        absorbed = dot(head_rows[:, h, :NOPE], up_keys[:, h * NOPE : (h + 1) * NOPE], ((1,), (1,))).astype(BF16)
        aq = rotate(head_rows[:, h, NOPE:], cos_a, sin_a)
        q_parts.append(jnp.concatenate([absorbed, aq, jnp.zeros((rows, 128 - ROPE), BF16)], axis=-1))
    q_all = jnp.concatenate(q_parts, axis=0)
    keys = jnp.concatenate(pieces, axis=0)
    key_positions = jnp.concatenate([b * rows + jnp.arange(rows, dtype=jnp.int32) for b in blocks])
    s = dot(q_all, keys, ((1,), (1,))) * ((NOPE + ROPE) ** (-0.5))
    visible = key_positions[None, None, :] <= positions[None, :, None]
    s = jnp.where(visible, s.reshape(mla_local, rows, -1), -jnp.inf).reshape(mla_local * rows, -1)
    top = jnp.max(s, axis=-1, keepdims=True)
    e = jnp.exp(s - top)
    total = jnp.sum(e, axis=-1, keepdims=True)
    weighted = dot(e.astype(BF16), keys[:, :KVR])
    log_weight = (top + jnp.log(total))[:, 0].reshape(1, mla_local, rows)
    mean = (weighted / total).astype(BF16)
    mla_heads = jnp.concatenate(
        [
            dot(mean[h * rows : (h + 1) * rows], up_values[:, h * VDM : (h + 1) * VDM]).astype(BF16)
            for h in range(mla_local)
        ],
        axis=-1,
    )

    for h in range(ret_local):
        cross = dot(rq[h], carried[h].astype(BF16)) * (scale * jnp.exp(cumulative[h])[:, None])
        retained = intra[h] + cross
        norm = lax.rsqrt(jnp.mean(retained * retained, axis=-1, keepdims=True) + 1e-06)
        ret_heads.append((retained * norm * ret_gain[h * VD : (h + 1) * VD]).astype(BF16))
    ret_heads = jnp.concatenate(ret_heads, axis=-1)

    if fs_size == 2:
        near = dot(ret_heads, ret_out) + dot(mla_heads, mla_out)
        far = dot(ret_heads, far_ret) + dot(mla_heads, far_mla)
        first = lax.axis_index("fs") == 0
        partial = jnp.concatenate([jnp.where(first, near, far), jnp.where(first, far, near)], axis=1).astype(BF16)
    else:
        partial = (dot(ret_heads, far_ret) + dot(mla_heads, far_mla)).astype(BF16)
    tp_size = lax.axis_size("tp")
    if tp_size == 2:
        half = rows // 2
        mine = lax.dynamic_slice_in_dim(partial, core * half, half, 0)
        theirs = lax.dynamic_slice_in_dim(partial, (1 - core) * half, half, 0)
        mixed = (mine.astype(F32) + swap(theirs, "tp", 1).astype(F32)).astype(BF16)
    else:
        mixed = lax.psum_scatter(partial, "tp", scatter_dimension=0, tiled=True)
    return mixed[:, None, :], log_weight


def solution(mesh):
    in_specs = (
        P("sp", "fs", "tp"),
        P("sp", "fs", "tp"),
        P("sp", "fs", "tp"),
        P("fs", "tp", "sp"),
        P("tp"),
        P("sp", "fs", "tp"),
        P("sp", "fs", None),
        P("sp", "fs", None),
        P(),
        P(),
        P("tp", "fs"),
        P("tp", "fs"),
    )
    out_specs = (P(("sp", "tp"), "fs", None), P("fs", "tp", "sp"))
    small = mesh.shape["sp"] == 8 and mesh.shape["fs"] == 2 and mesh.shape["tp"] == 2
    body = with_kernels if small else on_device
    return jax.shard_map(body, mesh=mesh, in_specs=in_specs, out_specs=out_specs, check_vma=False)
```
